128 devices in a mesh: ep: 64 (over z, y, x), tp: 2 (over core).
Axes of the slice: x: 4, y: 4, z: 4, core: 2. Of those that a mesh axis runs over, the one named last changes fastest.
Arguments:
- tokens: bfloat16 [16384, 2048], P('ep'), may hold values from -16 to 16
- expert_ids: int32 [16384, 4], P('ep'), may hold values from 0 to 63, all different within a row; in each aligned block of 256 rows (0 to 255, 256 to 511, ...) at most 24 rows name the same one
- gates: float32 [16384, 4], P('ep'), may hold values from 0.05 to 0.6
- cotangent: bfloat16 [16384, 2048], P('ep'), may hold values from -16 to 16
- w_gate: bfloat16 [64, 2048, 512], P('ep', None, 'tp'), may hold values from -0.125 to 0.125
- w_up: bfloat16 [64, 2048, 512], P('ep', None, 'tp'), may hold values from -0.125 to 0.125
- w_down: bfloat16 [64, 512, 2048], P('ep', 'tp'), may hold values from -0.25 to 0.25
- sh_gate: bfloat16 [2048, 512], P(None, 'tp'), may hold values from -0.125 to 0.125
- sh_up: bfloat16 [2048, 512], P(None, 'tp'), may hold values from -0.125 to 0.125
- sh_down: bfloat16 [512, 2048], P('tp'), may hold values from -0.25 to 0.25
Outputs:
- token_grad: bfloat16 [16384, 2048], P('ep', 'tp')
- gate_grad: float32 [16384, 4], P('ep')
- expert_gate_grad: float32 [64, 2048, 512], P('ep', None, 'tp')
- expert_up_grad: float32 [64, 2048, 512], P('ep', None, 'tp')
- expert_down_grad: float32 [64, 512, 2048], P('ep', 'tp')
- shared_gate_grad: float32 [2048, 512], P('ep', 'tp')
- shared_up_grad: float32 [2048, 512], P('ep', 'tp')
- shared_down_grad: float32 [512, 2048], P('tp', 'ep')
- expert_gate_rows: float32 [64, 2048], P('ep')
- expert_up_rows: float32 [64, 2048], P('ep')
- expert_down_rows: float32 [64, 512], P('ep', 'tp')
- shared_gate_rows: float32 [2048], P('ep')
- shared_up_rows: float32 [2048], P('ep')
- shared_down_rows: float32 [512], P('tp')
The draws below stay inside these ranges and needn't reach their ends.
Inputs may be any that keep to these rules, and one draw needn't show every extreme that they name: `expert_ids`: each row names 4 different experts. Within each aligned block of 256 tokens no expert is named by more than 24 assignments, a bound that is reached in some blocks.
All inputs are finite; a program needn't handle non-finite values.
Results may differ from the reference program's by a relative error of at most 0.0085.
Values may be sent and summed in bfloat16 or wider, within the bound.
A program may use at most 128 MiB of HBM per device.

```python
import math
import jax
import jax.numpy as jnp
import numpy as np
from jax import lax

D = 2048
HID = 512
SH = 512
TOP_K = 4
TOK_DEV = 256
EXPERTS = 64
CAP = 24
TOKENS = 16384
N_TP = 2


def with_spikes(values, stream_key, source, target, parts, factor):
    def block_of(position):
        return (jnp.arange(values.shape[position]) // (values.shape[position] // parts)).reshape((-1,) + (1,) * (values.ndim - 1 - position))

    first = jax.random.permutation(stream_key, parts)[block_of(target)]
    second = (block_of(target) + parts // 2) % parts
    return jnp.where((block_of(source) == first) | (block_of(source) == second), factor * values, values)


def levels(stream_key, shape, split, least, high):
    def one(dim, shards_of):
        steps = jax.random.uniform(jax.random.fold_in(jax.random.fold_in(stream_key, 6), dim), (shards_of,), jnp.float32, least / len(split), high / len(split))
        return jnp.repeat(jnp.exp(steps), shape[dim] // shards_of).reshape((-1,) + (1,) * (len(shape) - dim - 1))

    loudness = one(*split[0])
    for cut in split[1:]:
        loudness = loudness * one(*cut)
    return loudness


def deal_out(stream_key, own, number, rows, amount, top, reach, skew):
    ranking = jax.random.permutation(stream_key, amount)
    crowded, ordinary = load_shares(amount, rows * top, reach, skew, True), load_shares(amount, rows * top, reach, skew, False)
    places = jnp.arange(amount)

    def named(sizes, offset_by):
        used = int((sizes > 0).sum())
        fixed = max(1, used // 4)
        passed = fixed + (places - fixed + offset_by * (used - fixed)) % max(1, amount - fixed)
        return jnp.zeros((amount,), jnp.int32).at[ranking[jnp.where(places < fixed, places, passed)]].set(jnp.asarray(sizes, jnp.int32))

    sizes = jnp.where(number % 4 == 0, named(crowded, number // 4), named(ordinary, number - number // 4 - 1))
    mixed = jax.random.permutation(jax.random.fold_in(own, 3), amount)
    giver, sink = mixed[0:amount // 2 * 2:2], mixed[1:amount // 2 * 2:2]
    room = jnp.minimum(sizes[giver] - 1, reach - sizes[sink]) // 2
    room = jnp.where((giver == ranking[0]) | (sink == ranking[0]) | (sizes[sink] == 0), 0, jnp.maximum(room, 0))
    passed = jax.random.randint(jax.random.fold_in(own, 4), (amount // 2,), 0, 1 << 20) % (room + 1)
    sizes = sizes.at[giver].add(-passed).at[sink].add(passed)
    members = jnp.searchsorted(jnp.cumsum(sizes), jnp.arange(rows * top), side="right").astype(jnp.int32)
    grid = members.reshape(top, rows).T
    grid = grid[jax.random.permutation(jax.random.fold_in(own, 1), rows)]
    offset_by = jax.random.randint(jax.random.fold_in(own, 2), (rows, 1), 0, top)
    return jnp.take_along_axis(grid, (jnp.arange(top)[None, :] + offset_by) % top, axis=1)


def load_shares(count, total, most, skew, full):
    weights = [(1 << 20) // math.isqrt(grade ** skew) + 1 for grade in range(1, count + 1)]
    largest = most if full else min(most, max(-(-total // count), total * weights[0] // sum(weights)))
    least = 1 if total - largest >= count - 1 else 0
    given, spare = [largest] + [least] * (count - 1), total - largest - least * (count - 1)
    while spare > 0:
        movable = [i for i in range(1, count) if given[i] < largest] or [i for i in range(1, count) if given[i] < most]
        mass, remaining = sum([weights[i] for i in movable]), spare
        for i in movable:
            addition = min(most - given[i], max(1, remaining * weights[i] // mass), spare)
            given[i] = given[i] + addition
            spare = spare - addition
    return np.array(given)


def bell_draw(key, shape, deviation, reach, shards=(), kind=jnp.bfloat16):
    array = deviation * jax.random.normal(key, shape, jnp.float32)
    if shards:
        array = array * levels(key, shape, shards, -0.22, 0.18)
    return jnp.clip(array, -reach, reach).astype(kind)


def noise_with(key, extent, deviation, bound, cuts, heavy, kind=jnp.bfloat16):
    values = deviation * jax.random.normal(key, extent, jnp.float32)
    if cuts:
        values = values * levels(key, extent, cuts, -0.22, 0.18)
    return jnp.clip(with_spikes(values, jax.random.fold_in(key, 3), *heavy), -bound, bound).astype(kind)


def setup_inputs(seed: int = 0) -> dict:
    keys = jax.random.split(jax.random.key(seed), 11)
    tokens = noise_with(keys[0], (TOKENS, D), 1.0, 16.0, ((0, 64),), (0, 1, 64, 4.0))
    expert_ids_keys = jax.random.split(jax.random.fold_in(keys[1], 1), TOKENS // TOK_DEV)
    expert_ids_turns = jax.random.permutation(jax.random.fold_in(keys[1], 3), TOKENS // TOK_DEV)
    expert_ids = jax.vmap(lambda own, number: deal_out(jax.random.fold_in(keys[1], 2), own, number, TOK_DEV, EXPERTS, TOP_K, CAP, 2))(expert_ids_keys, expert_ids_turns).reshape((TOKENS, TOP_K))
    gates = jnp.clip(0.05 + 0.55 * jax.random.uniform(keys[2], (TOKENS, TOP_K), jnp.float32) ** levels(keys[2], (TOKENS, TOP_K), ((0, 64),), -0.2, 0.2), 0.05, 0.6)
    cotangent = noise_with(keys[3], (TOKENS, D), 1.0, 16.0, ((0, 64),), (0, 1, 64, 4.0))
    w_gate = bell_draw(keys[4], (EXPERTS, D, HID), D ** -0.5, 0.125, ((0, 64), (2, 2)))
    w_up = bell_draw(keys[5], (EXPERTS, D, HID), D ** -0.5, 0.125, ((0, 64), (2, 2)))
    w_down = bell_draw(keys[6], (EXPERTS, HID, D), HID ** -0.5, 0.25, ((0, 64), (1, 2)))
    sh_gate = bell_draw(keys[7], (D, SH), D ** -0.5, 0.125, ((1, 2),))
    sh_up = bell_draw(keys[8], (D, SH), D ** -0.5, 0.125, ((1, 2),))
    sh_down = bell_draw(keys[9], (SH, D), SH ** -0.5, 0.25, ((0, 2),))
    return dict(tokens=tokens, expert_ids=expert_ids, gates=gates, cotangent=cotangent, w_gate=w_gate, w_up=w_up, w_down=w_down, sh_gate=sh_gate, sh_up=sh_up, sh_down=sh_down)


def silu_parts(pre):
    sigmoid = jax.nn.sigmoid(pre)
    return pre * sigmoid, sigmoid * (1.0 + pre * (1.0 - sigmoid))


def halves_sum(left_a, right_a, left_b, right_b, pieces):
    step_cols = left_a.shape[1] // pieces
    total = jnp.zeros((left_a.shape[0], right_a.shape[0]), jnp.float32)
    for piece in range(pieces):
        first_col = piece * step_cols
        part = jnp.dot(left_a[:, first_col:first_col + step_cols], right_a[:, first_col:first_col + step_cols].T, preferred_element_type=jnp.float32)
        part = part + jnp.dot(left_b[:, first_col:first_col + step_cols], right_b[:, first_col:first_col + step_cols].T, preferred_element_type=jnp.float32)
        total = total + lax.optimization_barrier(part.astype(jnp.bfloat16)).astype(jnp.float32)
    return total


def backward_rows(inputs, cot_rows, w_g, w_u, w_d):
    gate_pre = jnp.dot(inputs, w_g, preferred_element_type=jnp.float32)
    up_pre = jnp.dot(inputs, w_u, preferred_element_type=jnp.float32)
    active, slope = silu_parts(gate_pre)
    hidden = (active * up_pre).astype(jnp.bfloat16)
    hidden_cot = jnp.dot(cot_rows, w_d.T, preferred_element_type=jnp.float32)
    gate_sum = jnp.sum(hidden.astype(jnp.float32) * hidden_cot, axis=1)
    d_gate = (hidden_cot * up_pre * slope).astype(jnp.bfloat16)
    d_up = (hidden_cot * active).astype(jnp.bfloat16)
    grad_g = jnp.dot(inputs.T, d_gate, preferred_element_type=jnp.float32)
    grad_u = jnp.dot(inputs.T, d_up, preferred_element_type=jnp.float32)
    grad_d = jnp.dot(hidden.T, cot_rows, preferred_element_type=jnp.float32)
    rows = halves_sum(d_gate, w_g, d_up, w_u, N_TP)
    return grad_g, grad_u, grad_d, rows, gate_sum


def reference(tokens, expert_ids, gates, cotangent, w_gate, w_up, w_down, sh_gate, sh_up, sh_down):
    per_dev = TOK_DEV * TOP_K
    assign = TOKENS * TOP_K
    slots = EXPERTS * CAP
    flat_ids = expert_ids.reshape(EXPERTS, per_dev).astype(jnp.int32)
    onehot = (flat_ids[:, :, None] == jnp.arange(EXPERTS, dtype=jnp.int32)[None, None, :]).astype(jnp.int32)
    slot_rank = jnp.sum((jnp.cumsum(onehot, axis=1) - 1) * onehot, axis=2)
    sources = jnp.arange(EXPERTS, dtype=jnp.int32)[:, None]
    slot_row = (flat_ids * slots + sources * CAP + slot_rank).reshape(assign).astype(jnp.int32)
    slot_table = jnp.full((EXPERTS * slots,), assign, jnp.int32).at[slot_row].set(jnp.arange(assign, dtype=jnp.int32))
    filled = slot_table < assign
    source = jnp.minimum(slot_table, assign - 1)
    token_row = (source // TOP_K).astype(jnp.int32)
    slot_gate = jnp.where(filled, gates.reshape(assign)[source], jnp.zeros((), jnp.float32))

    def one_expert(packed):
        rows_index, gate_col, keep, w_g, w_u, w_d = packed
        inputs = jnp.where(keep[:, None], tokens[rows_index], jnp.zeros((), tokens.dtype))
        cot_rows = (gate_col[:, None] * cotangent[rows_index].astype(jnp.float32)).astype(jnp.bfloat16)
        return backward_rows(inputs, cot_rows, w_g, w_u, w_d)

    grad_g, grad_u, grad_d, slot_rows, gate_sums = lax.map(one_expert, (token_row.reshape(EXPERTS, slots), slot_gate.reshape(EXPERTS, slots), filled.reshape(EXPERTS, slots), w_gate, w_up, w_down))
    flat_rows = slot_rows.reshape(EXPERTS * slots, D)
    picks = slot_row.reshape(TOKENS, TOP_K)
    routed = jnp.zeros((TOKENS, D), jnp.float32)
    for column in range(TOP_K):
        routed = routed + flat_rows[picks[:, column]].astype(jnp.float32)
    gate_grad = gate_sums.reshape(EXPERTS * slots)[picks] / gates
    shared_g, shared_u, shared_d, shared_rows, unused = backward_rows(tokens, cotangent, sh_gate, sh_up, sh_down)
    token_grad = (routed + shared_rows).astype(jnp.bfloat16)
    return (token_grad, gate_grad, grad_g, grad_u, grad_d, shared_g, shared_u, shared_d,
            jnp.sum(grad_g * grad_g, axis=2), jnp.sum(grad_u * grad_u, axis=2), jnp.sum(grad_d * grad_d, axis=2),
            jnp.sum(shared_g * shared_g, axis=1), jnp.sum(shared_u * shared_u, axis=1), jnp.sum(shared_d * shared_d, axis=1))
```

```python
import functools

import jax
import jax.numpy as jnp
from jax import lax
from jax.experimental import pallas as pl
from jax.experimental.pallas import tpu as pltpu
from jax.sharding import PartitionSpec as P

F32 = jnp.float32
BF16 = jnp.bfloat16
MESH_ID = pl.DeviceIdType.MESH
CAP = 24
NEP = 64
CHUNKS = 4
BLK = NEP // CHUNKS
ROWS = NEP * CAP
CR = BLK * CAP


AXES = ((2, 1, 0), (1, 0, 2), (0, 2, 1))
WIDE = (768, 512, 768)
BACK = (384, 384, 256)
B_AT = (0, 384, 768)
R_AT = (0, 768, 1280)
ORDER = (0, 1, 3, 2)


def place(me):
    return lax.rem(me, 4), lax.rem(lax.div(me, 4), 4), lax.div(me, 16)


def shifted(me, offs):
    x, y, z = (lax.rem(c + o, 4) for c, o in zip(place(me), offs))
    return z * 16 + y * 4 + x


def target(me, k):
    return shifted(me, place(k))


def origin(me, k):
    return shifted(me, tuple(4 - o for o in place(k)))


def nn(a, b):
    return lax.dot_general(a, b, (((1,), (0,)), ((), ())), preferred_element_type=F32)


def nt(a, b):
    return lax.dot_general(a, b, (((1,), (1,)), ((), ())), preferred_element_type=F32)


def tn(a, b):
    return lax.dot_general(a, b, (((0,), (0,)), ((), ())), preferred_element_type=F32)


def nonlinear(gp, up, hc):
    s = jax.nn.sigmoid(gp)
    act = gp * s
    slope = s * (1.0 + gp * (1.0 - s))
    hid = (act * up).astype(BF16)
    dg = (hc * up * slope).astype(BF16)
    du = (hc * act).astype(BF16)
    return hid, dg, du


def kernel(
    ids, gates, order, tok_h, cot_h, wg_h, wu_h, wd_h, sg_h, su_h, sd_h,
    o_tok, o_gate, o_rank, o_gg, o_gu, o_gd, o_nrm, o_dn, o_rs, o_sn, o_sdn,
    meta, meta_in, pick, slot_gate, tok, cot, wg, wu, wd, sg, su, sd,
    raw, b0, b1, b2, c0, c1, c2, w0, w1, w2, v0, v1, v2,
    hid_b, dg_b, du_b, rc0, rc1, rc2, rb0, rb1, rb2, s_r0, s_r1, s_r2,
    gpart, gother, g1, g2, g3, stage, nrm, nrm_o, sn, sn_o,
    sh_own, sh_give, sh_got, sh_sum, r0, r1, r2, q0, q1, q2, p1, p2, p3, dnb,
    a_s, a_r, i_s, i_r, d_s, d_r, k_s, k_r, f_s, f_r, x_s, x_r,
    b_s, b_r, y_s, y_r, z_s, z_r, l_s,
    g_s, g_r, t_s, t_r, n_s, n_r, st_s, e_s, e_r, w_s,
):
    out_b, mid, own, oth = (b0, b1, b2), (c0, c1, c2), (w0, w1, w2), (v0, v1, v2)
    rc, rb, s_r = (rc0, rc1, rc2), (rb0, rb1, rb2), (s_r0, s_r1, s_r2)
    me = lax.axis_index("ep")
    h = lax.axis_index("tp")
    mx, my, mz = place(me)
    mate = {"tp": 1 - h}
    width = tok.shape[1] // 2
    half = width // 2

    loads = [
        pltpu.make_async_copy(a, b, w_s.at[i])
        for i, (a, b) in enumerate(
            ((tok_h, tok), (cot_h, cot), (sg_h, sg), (su_h, su), (sd_h, sd), (wg_h, wg), (wu_h, wu), (wd_h, wd))
        )
    ]
    for cp in loads:
        cp.start()
    bar = pltpu.get_barrier_semaphore()

    def axis_peer(axis, d):
        x, y, z = mx, my, mz
        if axis == 0:
            x = lax.rem(x + d, 4)
        elif axis == 1:
            y = lax.rem(y + d, 4)
        else:
            z = lax.rem(z + d, 4)
        return x, y, z, z * 16 + y * 4 + x

    def peer(axis, d):
        return {"ep": axis_peer(axis, d)[3]}

    for axis in range(3):
        for d in range(1, 4):
            pl.semaphore_signal(bar, inc=1, device_id=peer(axis, d), device_id_type=MESH_ID)
    pl.semaphore_signal(bar, inc=1, device_id=mate, device_id_type=MESH_ID)

    def remote(src, dst, s, r, dev):
        return pltpu.make_async_remote_copy(
            src_ref=src, dst_ref=dst, send_sem=s, recv_sem=r, device_id=dev, device_id_type=MESH_ID
        )

    def flat(v):
        return v.reshape(-1, v.shape[-1])

    def blocks(v, *lead):
        return v.reshape(*lead, CAP, v.shape[-1])

    every = slice(None)

    def col(lo, n):
        return pl.ds(pl.multiple_of(h * width + lo, 128), n)

    raw_parts = (
        (0, tok, 0, 768, 0), (1, tok, 768, 256, 0), (1, cot, 0, 256, 256), (2, cot, 256, 768, 0),
    )

    def gather_copies(d):
        cps = []
        for i, (q, src, lo, n, at) in enumerate(raw_parts):
            cps.append((q, remote(
                src.at[:, col(lo, n)], raw.at[pl.ds((d - 1) * 256, 256), pl.ds(R_AT[q] + at, n)],
                a_s.at[d - 1, i], a_r.at[d - 1, i], peer(AXES[q][0], d),
            )))
        return cps

    def meta_copy(q, d):
        return remote(
            meta.at[q, d], meta_in.at[q, d - 1], i_s.at[q, d - 1], i_r.at[q, d - 1], peer(AXES[q][0], d)
        )

    def first_copy(q, d, e):
        return remote(
            out_b[q].at[e - 1, d], mid[q].at[d, e],
            d_s.at[q, d, e - 1], d_r.at[q, d, e - 1], peer(AXES[q][1], e),
        )

    def second_copies(q, c):
        out = []
        for g in (1, 3, 2, 0) if q != 1 else (c,):
            m, o = mid[q], own[q]
            src = (m.at[c, :, g], m.at[:, :, c], m.at[:, c, g])[q]
            dst = (o.at[c, :, g], o.at[c], o.at[c, g])[q]
            if g == 0:
                out.append((g, pltpu.make_async_copy(src, dst, k_s.at[q, c, 0])))
            else:
                out.append((g, remote(src, dst, k_s.at[q, c, g], k_r.at[q, c, g], peer(AXES[q][2], g))))
        return out

    def forward(q, c):
        return remote(own[q].at[c], oth[q].at[c], f_s.at[q, c], f_r.at[q, c], mate)

    firsts = set()

    def second(q, c):
        for d in (c,) if q == 0 else range(4):
            for e in (c,) if q == 2 else range(4):
                if e > 0 and (q, d, e) not in firsts:
                    firsts.add((q, d, e))
                    first_copy(q, d, e).wait_recv()
        for _, cp in second_copies(q, c):
            cp.start()

    n_tok = tok.shape[0]
    earlier = lax.broadcasted_iota(jnp.int32, (n_tok, n_tok), 0)
    later = lax.broadcasted_iota(jnp.int32, (n_tok, n_tok), 1)
    before = jnp.where(later > earlier, 1.0, 0.0).astype(BF16)
    for q in range(3):
        named = jnp.zeros((NEP, n_tok), F32)
        gate_t = jnp.zeros((NEP, n_tok), F32)
        for j in range(4):
            hit = ids[j:j + 1] == order[q]
            named = jnp.where(hit, 1.0, named)
            gate_t = jnp.where(hit, gates[j:j + 1], gate_t)
        rank_t = jnp.where(named > 0.0, nn(named.astype(BF16), before), -1.0)
        if q == 0:
            o_rank[...] = rank_t
        for d in range(4):
            meta[q, d, 0] = rank_t[d * 16:(d + 1) * 16]
            meta[q, d, 1] = gate_t[d * 16:(d + 1) * 16]

    for cp in loads[:2]:
        cp.wait()
    pl.semaphore_wait(bar, 10)
    sends = []
    for d in (1, 3, 2):
        for q in range(3):
            sends.append(meta_copy(q, d))
        sends.extend(cp for _, cp in gather_copies(d))
    n_near = 2 * len(sends) // 3
    for cp in sends[:n_near]:
        cp.start()

    slot_no = lax.broadcasted_iota(jnp.int32, (CAP, n_tok), 0).astype(F32)

    def place_rows(q, d, with_gate):
        ref = meta.at[q, 0] if d == 0 else meta_in.at[q, d - 1]
        for k in range(16):
            filled = ref[0, k:k + 1] == slot_no
            pick[k * CAP:(k + 1) * CAP] = jnp.where(filled, 1.0, 0.0).astype(BF16)
            if with_gate:
                slot_gate[k * CAP:(k + 1) * CAP] = jnp.sum(
                    jnp.where(filled, ref[1, k:k + 1], 0.0), axis=1, keepdims=True
                )

    def put(q, d, cols, v):
        v = blocks(v, 4, 4).astype(BF16)
        mid[q][d, 0, :, :, cols] = v[0]
        for e in range(1, 4):
            out_b[q][e - 1, d, :, :, cols] = v[e]

    for cp in loads[2:]:
        cp.wait()
    gp = nn(tok[...], sg[...])
    up = nn(tok[...], su[...])
    hc = nt(cot[...], sd[...])
    s_hid, s_dg, s_du = nonlinear(gp, up, hc)
    tile = 512
    tiles = tok.shape[1] // tile
    for i in range(tiles):
        cs = slice(i * tile, (i + 1) * tile)
        t_t = tok[:, cs]
        r0[i] = tn(t_t, s_dg).astype(BF16)
        r1[i] = tn(t_t, s_du).astype(BF16)
        r2[4 * i:4 * i + 4] = tn(cot[:, cs], s_hid).astype(BF16).reshape(4, 128, 256)

    def rs_copies(phase):
        out = []
        for d in (1, 3, 2):
            for a in range(3):
                axis = AXES[a][phase]
                x, y, z, dev = axis_peer(axis, d)
                if phase == 0:
                    src = (r0.at[z], r1.at[:, pl.ds(pl.multiple_of(y * 128, 128), 128)],
                           r2.at[:, pl.ds(pl.multiple_of(x * 32, 32), 32)])[a]
                    dst = (q0, q1, q2)[a].at[d - 1]
                elif phase == 1:
                    src = (p1.at[0, pl.ds(pl.multiple_of(y * 4, 4), 4)], p1.at[1, pl.ds(pl.multiple_of(x * 4, 4), 4)],
                           p1.at[2, pl.ds(pl.multiple_of(z * 4, 4), 4)])[a]
                    dst = p2.at[a, d]
                else:
                    src = p2.at[a, 0, (x, z, y)[a]]
                    dst = p3.at[a, d - 1]
                i = (phase * 3 + d - 1) * 3 + a
                out.append(remote(src, dst, t_s.at[i], t_r.at[i], {"ep": dev}))
        return out

    def produce(d):
        for q in range(3):
            if d > 0:
                meta_copy(q, d).wait_recv()
                for qq, cp in gather_copies(d):
                    if qq == q:
                        cp.wait_recv()
            place_rows(q, d, q > 0)
            for qq, src, lo, n, at in raw_parts:
                if qq != q:
                    continue
                for j in range(0, n, 256):
                    if d == 0:
                        x = src[:, col(lo + j, 256)]
                    else:
                        x = raw[(d - 1) * 256:d * 256, R_AT[q] + at + j:R_AT[q] + at + j + 256]
                    v = nn(pick[...], x)
                    if src is cot:
                        v = slot_gate[...] * v
                    put(q, d, slice(at + j, at + j + 256), v)
            for e in range(1, 4):
                first_copy(q, d, e).start()

    produce(0)
    for cp in sends[n_near:]:
        cp.start()
    for i in range(2):
        cols = pl.ds(pl.multiple_of(h * width + i * half, 128), half)
        r = pl.ds(pl.multiple_of(h * width + i * half, 128), half)
        sh_own[:, i * half:(i + 1) * half] = (
            nt(s_dg, sg[r]) + nt(s_du, su[r])
        ).astype(BF16)
        r = pl.ds(pl.multiple_of((1 - h) * width + i * half, 128), half)
        sh_give[:, i * half:(i + 1) * half] = (
            nt(s_dg, sg[r]) + nt(s_du, su[r])
        ).astype(BF16)
    sh_cp = remote(sh_give, sh_got, e_s.at[0], e_r.at[0], mate)
    sh_cp.start()

    produce(1)
    produce(3)
    produce(2)
    rs0 = rs_copies(0)
    second(2, 0)
    second(0, 0)

    for q, c in ((1, 0), (0, 1), (1, 1), (1, 3), (2, 1), (1, 2), (0, 3), (2, 3)):
        second(q, c)

    def arrive(c):
        for q in range(3):
            for g, cp in second_copies(q, c):
                if g > 0:
                    cp.wait_recv()
                else:
                    cp.wait()
            forward(q, c).start()

    def cross(c):
        out = []
        for i in range(4):
            buf, at = give_at(c, i)
            dst = raw.at[pl.ds((c // 2) * CR, CR), pl.ds((c % 2) * width + i * 256, 256)]
            out.append(remote(buf.at[pl.ds(at, CR)], dst, x_s.at[c, i], x_r.at[c, i], mate))
        return out

    def give_at(c, i):
        n = ORDER.index(c) % 2 * 4 + i
        return (sg, su)[n // 5], n % 5 * CR

    def back_at(q, c):
        if q == 0:
            return out_b[0], c % 3, 384 * (c // 3)
        if c == 3:
            return out_b[2], q - 1 if q == 1 else 1, 256
        return out_b[q], c, 0

    def rows_of(base, lo, n):
        return pl.ds(pl.multiple_of(base * width + lo, 128), n)

    def compute(c):
        rows = pl.ds(c * CR, CR)
        for q in range(3):
            forward(q, c).wait_recv()
        gp = up = hc = None
        for base, buf in ((h, own), (1 - h, oth)):
            for lo, n, x in ((0, 768, flat(buf[0][c])), (768, 256, flat(buf[1][c, :, :, :, :256]))):
                r = rows_of(base, lo, n)
                g, u = nn(x, wg[r]), nn(x, wu[r])
                gp, up = (g, u) if gp is None else (gp + g, up + u)
            for lo, n, x in ((0, 256, flat(buf[1][c, :, :, :, 256:])), (256, 768, flat(buf[2][c]))):
                t = nt(x, wd[:, rows_of(base, lo, n)])
                hc = t if hc is None else hc + t
        hid, dg, du = nonlinear(gp, up, hc)
        hid_b[rows] = hid
        dg_b[rows] = dg
        du_b[rows] = du
        gsum = jnp.sum(hid.astype(F32) * hc, axis=1, keepdims=True).reshape(BLK, CAP, 1)
        lane = lax.broadcasted_iota(jnp.int32, (BLK, CAP, 128), 2)
        rank = lax.broadcasted_iota(jnp.int32, (BLK, CAP, 128), 1)
        packed = jnp.sum(jnp.where(lane == rank, gsum, 0.0), axis=1)
        for i in range(BLK):
            gpart[c, i // 4, i % 4] = packed[i:i + 1]
        if ORDER.index(c) >= 2:
            for cp in cross(ORDER[ORDER.index(c) - 2]):
                cp.wait_send()
        for i, cp in enumerate(cross(c)):
            buf, at = give_at(c, i)
            r = pl.ds(pl.multiple_of((1 - h) * width + i * 256, 256), 256)
            buf[at:at + CR] = (nt(dg, wg[r]) + nt(du, wu[r])).astype(BF16)
            cp.start()
        for q in range(3):
            r = rows_of(h, B_AT[q], BACK[q])
            buf, b, lo = back_at(q, c)
            buf[b, :, :, :, lo:lo + BACK[q]] = blocks(nt(dg, wg[r]) + nt(du, wu[r]), 4, 4).astype(BF16)

    def back_copies(q, c):
        out = []
        buf, b, lo = back_at(q, c)
        src = buf.at[b, :, :, :, pl.ds(lo, BACK[q])]
        for g in (1, 3, 2, 0) if q != 1 else (c,):
            s_g = (src.at[:, g], src, src.at[g])[q]
            v = rc[q]
            dst = (v.at[c, :, g], v.at[:, :, c], v.at[:, c, g])[q]
            if g == 0:
                out.append((g, pltpu.make_async_copy(s_g, dst, l_s.at[q, c])))
            else:
                to = peer(AXES[q][2], 4 - g)
                out.append((g, remote(s_g, dst, b_s.at[q, c, g], b_r.at[q, c, g], to)))
        return out

    def finish(c):
        for cp in cross(c):
            cp.wait_recv()
        for q in range(3):
            n = BACK[q]
            buf, b, lo = back_at(q, c)
            at = c % 2 * width + B_AT[q]
            buf[b, :, :, :, lo:lo + n] = (
                buf[b, :, :, :, lo:lo + n].astype(F32)
                + blocks(raw[(c // 2) * CR:(c // 2 + 1) * CR, at:at + n].astype(F32), 4, 4)
            ).astype(BF16)
        for q in range(3):
            for _, cp in back_copies(q, c):
                cp.start()

    def back2_copies(q, c):
        out = []
        v, w = rc[q], rb[q]
        for e in (1, 3, 2, 0) if q != 2 else (c,):
            at = ((c, e), (every, e, c), (every, e))[q]
            if e == 0:
                out.append((e, pltpu.make_async_copy(v.at[at], w.at[at], l_s.at[q, 4 + c])))
            else:
                to = peer(AXES[q][1], 4 - e)
                out.append((e, remote(v.at[at], w.at[at], y_s.at[q, c, e], y_r.at[q, c, e], to)))
        return out

    def legs(c):
        for q in (1, 2, 0):
            for g, cp in back_copies(q, c):
                if g > 0:
                    cp.wait_recv()
                else:
                    cp.wait()
            for _, cp in back2_copies(q, c):
                cp.start()

    for q in range(3):
        for d in range(4):
            for e in range(1, 4):
                first_copy(q, d, e).wait_send()
    for n, c in enumerate(ORDER):
        arrive(c)
        for q, cc in ((), ((0, 2), (2, 2)), (), ())[n]:
            second(q, cc)
        for a in ((), (0,), (1, 2), ())[n]:
            for cp in rs0[a::3]:
                cp.start()
        if n >= 1:
            finish(ORDER[n - 1])
        compute(c)
        if n == 2:
            legs(0)
    g_cp = remote(gpart, gother, e_s.at[1], e_r.at[1], mate)
    g_cp.start()
    finish(ORDER[-1])
    legs(1)

    def leg2_done(q, c):
        for e, cp in back2_copies(q, c):
            if e > 0:
                cp.wait_recv()
            else:
                cp.wait()

    def back3_copy(q, d):
        return remote(
            raw.at[pl.ds((d - 1) * 256, 256), pl.ds(R_AT[q], BACK[q])], s_r[q].at[d - 1],
            z_s.at[q, d], z_r.at[q, d], peer(AXES[q][0], 4 - d),
        )

    def leg3(q, d):
        place_rows(q, d, False)
        v = tn(pick[...], flat(rb[q][d]))
        if d > 0:
            raw[(d - 1) * 256:d * 256, R_AT[q]:R_AT[q] + BACK[q]] = v.astype(BF16)
            back3_copy(q, d).start()
        else:
            sh_sum[:, B_AT[q]:B_AT[q] + BACK[q]] = v

    def near_rows():
        for d in (0, 1, 3):
            leg2_done(0, d)
            leg3(0, d)

    def far_rows():
        for q in (1, 2):
            for c in ORDER:
                leg2_done(q, c)
            for d in (1, 3, 2, 0):
                leg3(q, d)
        leg2_done(0, 2)
        leg3(0, 2)

    def f(v):
        return v.astype(F32)

    def scatter2():
        for cp in rs0:
            cp.wait()
        s0 = f(r0[mz]) + f(q0[0]) + f(q0[1]) + f(q0[2])
        p1[0] = s0.reshape(16, 32, 256).astype(BF16)
        s1 = (f(r1[:, pl.ds(pl.multiple_of(my * 128, 128), 128)]) + f(q1[0]) + f(q1[1]) + f(q1[2])).reshape(4, 4, 32, 256)
        for i in range(4):
            for j in range(4):
                p1[1, 4 * j + i] = s1[i, j].astype(BF16)
        s2 = f(r2[:, pl.ds(pl.multiple_of(mx * 32, 32), 32)]) + f(q2[0]) + f(q2[1]) + f(q2[2])
        p1[2] = s2.astype(BF16)
        for cp in rs_copies(1):
            cp.start()

    def scatter3():
        for cp in rs_copies(1):
            cp.wait()
        for a in range(3):
            own_i = (my, mx, mz)[a]
            p2[a, 0] = (
                f(p1[a, pl.ds(pl.multiple_of(own_i * 4, 4), 4)]) + f(p2[a, 1]) + f(p2[a, 2]) + f(p2[a, 3])
            ).astype(BF16)
        for cp in rs_copies(2):
            cp.start()

    gates_on = (gother, g1, g2, g3)

    def gate_copies(leg):
        out = []
        for g in range(1, 4):
            at = ((every, every, g), (every, g), (g,))[leg]
            src, dst = gates_on[leg].at[at], gates_on[leg + 1].at[at]
            out.append(remote(src, dst, g_s.at[leg, g], g_r.at[leg, g], peer(leg, 4 - g)))
        return out

    def gate_leg(leg):
        if leg == 0:
            g_cp.wait()
            gother[...] = gpart[...] + gother[...]
        else:
            for cp in gate_copies(leg - 1):
                cp.wait()
        at = ((every, every, 0), (every, 0), (0,))[leg]
        gates_on[leg + 1][at] = gates_on[leg][at]
        for cp in gate_copies(leg):
            cp.start()

    sn_cp = remote(sn, sn_o, e_s.at[3], e_r.at[3], mate)

    def spread(leg):
        return [
            remote(dnb.at[leg, 0], dnb.at[leg, g], n_s.at[leg, g], n_r.at[leg, g], peer(leg, g))
            for g in range(1, 4)
        ]

    def spread_leg(leg):
        if leg > 0:
            for cp in spread(leg - 1):
                cp.wait()
            dnb[leg, 0] = dnb[leg - 1, 0] + dnb[leg - 1, 1] + dnb[leg - 1, 2] + dnb[leg - 1, 3]
        if leg < 3:
            for cp in spread(leg):
                cp.start()

    def scatter_end():
        for cp in rs_copies(2):
            cp.wait()
        for a in range(3):
            own_i = (mx, mz, my)[a]
            v = f(p2[a, 0, own_i]) + f(p3[a, 0]) + f(p3[a, 1]) + f(p3[a, 2])
            o_rs[a] = v
            if a < 2:
                sn[a] = jnp.broadcast_to(jnp.sum(v * v, axis=1, keepdims=True), (32, 128))
            else:
                dnb[0, 0] = jnp.sum(v * v, axis=0, keepdims=True)
        sn_cp.start()
        spread_leg(0)

    ones = jnp.ones((8, 256), F32)

    def row_norm(g):
        return lax.dot_general(
            ones, g * g, (((1,), (1,)), ((), ())), preferred_element_type=F32, precision=lax.Precision.HIGHEST
        )

    n_t = width // 256

    def stage_copies(step, slot, f0):
        fr = pl.ds(f0, 256)
        return (
            pltpu.make_async_copy(stage.at[slot, 0], o_gg.at[fr], st_s.at[slot, 0]),
            pltpu.make_async_copy(stage.at[slot, 1], o_gu.at[fr], st_s.at[slot, 1]),
            pltpu.make_async_copy(stage.at[slot, 2], o_gd.at[:, fr], st_s.at[slot, 2]),
        )

    hid_all = hid_b[...]
    dn = jnp.zeros((8, 256), F32)
    pending = [None, None]
    AFTER = {
        0: (functools.partial(legs, 3), functools.partial(gate_leg, 0)),
        1: (functools.partial(legs, 2), scatter2),
        2: (near_rows, functools.partial(gate_leg, 1)),
        3: (far_rows, scatter3),
        4: (functools.partial(gate_leg, 2),),
        5: (scatter_end,),
        6: (functools.partial(spread_leg, 1),),
        7: (functools.partial(spread_leg, 2),),
    }
    for step in range(2 * n_t):
        slot = step % 2
        buf = own if step < n_t else oth
        i = step % n_t
        base = h if step < n_t else 1 - h
        f0 = pl.multiple_of(base * width + i * 256, 256)
        if pending[slot] is not None:
            for cp in pending[slot]:
                cp.wait()
        lhs = flat(buf[0][..., i * 256:(i + 1) * 256] if i < 3 else buf[1][..., :256])
        rhs = flat(buf[1][..., 256:] if i == 0 else buf[2][..., (i - 1) * 256:i * 256])
        grad1 = tn(lhs, dg_b[...])
        stage[slot, 0] = grad1
        nrm[0:8, pl.ds(f0, 256)] = row_norm(grad1)
        grad2 = tn(lhs, du_b[...])
        stage[slot, 1] = grad2
        nrm[8:16, pl.ds(f0, 256)] = row_norm(grad2)
        grad3 = tn(hid_all, rhs)
        stage[slot, 2] = grad3
        dn = dn + row_norm(grad3)
        pending[slot] = stage_copies(step, slot, f0)
        for cp in pending[slot]:
            cp.start()
        for fn in AFTER.get(step, ()):
            fn()
    o_dn[...] = dn
    nrm_cp = remote(nrm, nrm_o, e_s.at[2], e_r.at[2], mate)
    nrm_cp.start()

    nrm_cp.wait()
    o_nrm[...] = nrm[...] + nrm_o[...]
    sn_cp.wait()
    o_sn[...] = sn[...] + sn_o[...]
    sh_cp.wait()
    for cp in gate_copies(2):
        cp.wait()
    for k in range(NEP):
        o_gate[k:k + 1] = g3[k // 16, k // 4 % 4, k % 4]
    for q in range(3):
        cs = slice(B_AT[q], B_AT[q] + BACK[q])
        v = sh_sum[:, cs] + (f(sh_own[:, cs]) + f(sh_got[:, cs]))
        for d in range(1, 4):
            back3_copy(q, d).wait()
            v = v + f(s_r[q][d - 1])
        o_tok[:, cs] = v.astype(BF16)

    spread_leg(3)
    o_sdn[...] = dnb[3, 0]
    for cp in sends:
        cp.wait_send()
    for q in range(3):
        for c in range(CHUNKS):
            forward(q, c).wait_send()
            for g, cp in second_copies(q, c) + back_copies(q, c):
                if g > 0:
                    cp.wait_send()
            for e, cp in back2_copies(q, c):
                if e > 0:
                    cp.wait_send()
    for c in ORDER[2:]:
        for cp in cross(c):
            cp.wait_send()
    for cps in pending:
        for cp in cps:
            cp.wait()


def tail(
    ids, gates, order, rank, gate_sum, tok_in, nrm, dn, rs, sn, sdn, gg, gu, gd,
    o_tok, o_gate, o_gg, o_gu, o_gd, o_sg, o_su, o_sd, o_gn, o_un, o_dn, o_sgn, o_sun, o_sdn,
    bg, bu, bd, i_s, o_s,
):
    rows = bd.shape[0]
    parts = []
    for a, (src, buf, dst) in enumerate(((gg, bg, o_gg), (gu, bu, o_gu))):
        for i in range(2):
            r = pl.ds(i * 1024, 1024)
            parts.append((src.at[r], buf.at[r], dst.at[0, r]))
    for i in range(2):
        r = pl.ds(i * 128, 128)
        parts.append((gd.at[r], bd.at[r], o_gd.at[0, r]))
    ins = [pltpu.make_async_copy(a, b, i_s.at[i]) for i, (a, b, _) in enumerate(parts)]
    outs = [pltpu.make_async_copy(b, c, o_s.at[i]) for i, (_, b, c) in enumerate(parts)]
    for cp in ins:
        cp.start()
    o_tok[...] = tok_in[...]
    value = jnp.zeros(rank.shape, F32)
    for r in range(CAP):
        value = jnp.where(rank[...] == float(r), gate_sum[:, r:r + 1], value)
    for j in range(4):
        hit = ids[j:j + 1] == order[0]
        total = jnp.sum(jnp.where(hit, value, 0.0), axis=0, keepdims=True)
        o_gate[j:j + 1] = total / gates[j:j + 1]
    o_sg[...] = rs[0]
    o_su[...] = rs[1]
    o_sd[...] = rs[2].T
    o_gn[...] = nrm[0:1]
    o_un[...] = nrm[8:9]
    o_dn[...] = dn[0:1]
    o_sgn[...] = sn[0].T[0:1]
    o_sun[...] = sn[1].T[0:1]
    o_sdn[...] = sdn[...]
    for a, b in zip(ins, outs):
        a.wait()
        b.start()
    for b in outs:
        b.wait()


def local(tokens, expert_ids, gates, cotangent, w_gate, w_up, w_down, sh_gate, sh_up, sh_down):
    me = lax.axis_index("ep")
    rows, width = tokens.shape
    k = lax.broadcasted_iota(jnp.int32, (NEP, 1), 0)
    dist = place(k)[::-1]
    order = jnp.stack(
        [shifted(me, tuple(dist[AXES[q].index(axis)] for axis in range(3))) for q in range(3)]
    )
    ids_t, gates_t = expert_ids.T, gates.T

    vm = pl.BlockSpec(memory_space=pltpu.VMEM)
    hbm = pl.BlockSpec(memory_space=pl.ANY)
    half = width // 2
    dma = pltpu.SemaphoreType.DMA
    out = pl.pallas_call(
        kernel,
        out_shape=(
            jax.ShapeDtypeStruct((rows, half), BF16),
            jax.ShapeDtypeStruct((NEP, 128), F32),
            jax.ShapeDtypeStruct((NEP, rows), F32),
            jax.ShapeDtypeStruct((width, 256), F32),
            jax.ShapeDtypeStruct((width, 256), F32),
            jax.ShapeDtypeStruct((256, width), F32),
            jax.ShapeDtypeStruct((16, width), F32),
            jax.ShapeDtypeStruct((8, 256), F32),
            jax.ShapeDtypeStruct((3, 32, 256), F32),
            jax.ShapeDtypeStruct((2, 32, 128), F32),
            jax.ShapeDtypeStruct((1, 256), F32),
        ),
        in_specs=[vm] * 3 + [hbm] * 8,
        out_specs=(vm, vm, vm, hbm, hbm, hbm, vm, vm, vm, vm, vm),
        scratch_shapes=[
            pltpu.VMEM((3, 4, 2, 16, rows), F32),
            pltpu.VMEM((3, 3, 2, 16, rows), F32),
            pltpu.VMEM((CR, rows), BF16),
            pltpu.VMEM((CR, 1), F32),
            pltpu.VMEM((rows, width), BF16),
            pltpu.VMEM((rows, width), BF16),
            pltpu.VMEM((width, 256), BF16),
            pltpu.VMEM((width, 256), BF16),
            pltpu.VMEM((256, width), BF16),
            pltpu.VMEM((width, 256), BF16),
            pltpu.VMEM((width, 256), BF16),
            pltpu.VMEM((256, width), BF16),
            pltpu.VMEM((3 * rows, width), BF16),
            *[pltpu.VMEM((3, 4, 4, CAP, n), BF16) for n in WIDE],
            *[pltpu.VMEM((4, 4, 4, CAP, n), BF16) for n in WIDE],
            *[pltpu.VMEM((4, 4, 4, CAP, n), BF16) for n in WIDE],
            *[pltpu.VMEM((4, 4, 4, CAP, n), BF16) for n in WIDE],
            pltpu.VMEM((ROWS, 256), BF16),
            pltpu.VMEM((ROWS, 256), BF16),
            pltpu.VMEM((ROWS, 256), BF16),
            *[pltpu.VMEM((4, 4, 4, CAP, n), BF16) for n in BACK],
            *[pltpu.VMEM((4, 4, 4, CAP, n), BF16) for n in BACK],
            *[pltpu.VMEM((3, rows, n), BF16) for n in BACK],
            *[pltpu.VMEM((4, 4, 4, 1, 128), F32)] * 5,
            pltpu.VMEM((2, 3, 256, 256), F32),
            pltpu.VMEM((16, width), F32),
            pltpu.VMEM((16, width), F32),
            pltpu.VMEM((2, 32, 128), F32),
            pltpu.VMEM((2, 32, 128), F32),
            pltpu.VMEM((rows, half), BF16),
            pltpu.VMEM((rows, half), BF16),
            pltpu.VMEM((rows, half), BF16),
            pltpu.VMEM((rows, half), F32),
            pltpu.VMEM((4, 512, 256), BF16),
            pltpu.VMEM((4, 512, 256), BF16),
            pltpu.VMEM((16, 128, 256), BF16),
            pltpu.VMEM((3, 512, 256), BF16),
            pltpu.VMEM((3, 4, 128, 256), BF16),
            pltpu.VMEM((3, 16, 32, 256), BF16),
            pltpu.VMEM((3, 16, 32, 256), BF16),
            pltpu.VMEM((3, 4, 4, 32, 256), BF16),
            pltpu.VMEM((3, 3, 32, 256), BF16),
            pltpu.VMEM((4, 4, 1, 256), F32),
            dma((3, 4)), dma((3, 4)),
            dma((3, 3)), dma((3, 3)),
            dma((3, 4, 3)), dma((3, 4, 3)),
            dma((3, 4, 4)), dma((3, 4, 4)),
            dma((3, 4)), dma((3, 4)),
            dma((CHUNKS, 4)), dma((CHUNKS, 4)),
            dma((3, CHUNKS, 4)), dma((3, CHUNKS, 4)),
            dma((3, CHUNKS, 4)), dma((3, CHUNKS, 4)),
            dma((3, 4)), dma((3, 4)),
            dma((3, 8)),
            dma((3, 4)), dma((3, 4)),
            dma((27,)), dma((27,)),
            dma((3, 4)), dma((3, 4)),
            dma((2, 3)),
            dma((4,)), dma((4,)),
            dma((8,)),
        ],
        compiler_params=pltpu.CompilerParams(
            collective_id=0, has_side_effects=True, vmem_limit_bytes=67043328
        ),
    )(ids_t, gates_t, order, tokens, cotangent, w_gate[0], w_up[0], w_down[0], sh_gate, sh_up, sh_down)
    tok_grad, gate_sum, rank, gg, gu, gd, nrm, dn, rs, sn, sdn = out
    res = pl.pallas_call(
        tail,
        out_shape=(
            jax.ShapeDtypeStruct((rows, half), BF16),
            jax.ShapeDtypeStruct((4, rows), F32),
            jax.ShapeDtypeStruct((1, width, 256), F32),
            jax.ShapeDtypeStruct((1, width, 256), F32),
            jax.ShapeDtypeStruct((1, 256, width), F32),
            jax.ShapeDtypeStruct((32, 256), F32),
            jax.ShapeDtypeStruct((32, 256), F32),
            jax.ShapeDtypeStruct((256, 32), F32),
            jax.ShapeDtypeStruct((1, width), F32),
            jax.ShapeDtypeStruct((1, width), F32),
            jax.ShapeDtypeStruct((1, 256), F32),
            jax.ShapeDtypeStruct((1, 32), F32),
            jax.ShapeDtypeStruct((1, 32), F32),
            jax.ShapeDtypeStruct((1, 256), F32),
        ),
        in_specs=[vm] * 11 + [hbm] * 3,
        out_specs=(vm, vm, hbm, hbm, hbm) + (vm,) * 9,
        scratch_shapes=[
            pltpu.VMEM((width, 256), F32),
            pltpu.VMEM((width, 256), F32),
            pltpu.VMEM((256, width), F32),
            dma((6,)), dma((6,)),
        ],
    )(ids_t, gates_t, order, rank, gate_sum, tok_grad, nrm, dn, rs, sn, sdn, gg, gu, gd)
    return (res[0], res[1].T) + res[2:11] + (res[11][0], res[12][0], res[13][0])


def solution(mesh):
    placed = (
        P("ep", None),
        P("ep", None),
        P("ep", None),
        P("ep", None),
        P("ep", None, "tp"),
        P("ep", None, "tp"),
        P("ep", "tp", None),
        P(None, "tp"),
        P(None, "tp"),
        P("tp", None),
    )
    return jax.shard_map(
        local,
        mesh=mesh,
        in_specs=placed,
        out_specs=(
            P("ep", "tp"),
            P("ep", None),
            P("ep", None, "tp"),
            P("ep", None, "tp"),
            P("ep", "tp", None),
            P("ep", "tp"),
            P("ep", "tp"),
            P("tp", "ep"),
            P("ep", None),
            P("ep", None),
            P("ep", "tp"),
            P("ep"),
            P("ep"),
            P("tp"),
        ),
        check_vma=False,
    )
```

```python
import functools

import jax
import jax.numpy as jnp
from jax import lax
from jax.experimental import pallas as pl
from jax.experimental.pallas import tpu as pltpu
from jax.sharding import PartitionSpec as P

F32 = jnp.float32
BF16 = jnp.bfloat16
MESH_ID = pl.DeviceIdType.MESH
CAP = 24
NEP = 64
CHUNKS = 4
BLK = NEP // CHUNKS
ROWS = NEP * CAP
CR = BLK * CAP


AXES = ((2, 1, 0), (1, 0, 2), (0, 2, 1))
WIDE = (768, 512, 768)
BACK = (384, 384, 256)
B_AT = (0, 384, 768)
R_AT = (0, 768, 1280)
ORDER = (0, 1, 3, 2)


def place(me):
    return lax.rem(me, 4), lax.rem(lax.div(me, 4), 4), lax.div(me, 16)


def shifted(me, offs):
    x, y, z = (lax.rem(c + o, 4) for c, o in zip(place(me), offs))
    return z * 16 + y * 4 + x


def target(me, k):
    return shifted(me, place(k))


def origin(me, k):
    return shifted(me, tuple(4 - o for o in place(k)))


def named_in_order(me, q, n):
    k = lax.broadcasted_iota(jnp.int32, (NEP, n), 0)
    dist = ((k >> 4) & 3, (k >> 2) & 3, k & 3)
    x, y, z = ((c + dist[AXES[q].index(axis)]) & 3 for axis, c in enumerate(place(me)))
    return z * 16 + y * 4 + x


def nn(a, b):
    return lax.dot_general(a, b, (((1,), (0,)), ((), ())), preferred_element_type=F32)


def nt(a, b):
    return lax.dot_general(a, b, (((1,), (1,)), ((), ())), preferred_element_type=F32)


def tn(a, b):
    return lax.dot_general(a, b, (((0,), (0,)), ((), ())), preferred_element_type=F32)


def nonlinear(gp, up, hc):
    s = jax.nn.sigmoid(gp)
    act = gp * s
    slope = s * (1.0 + gp * (1.0 - s))
    hid = (act * up).astype(BF16)
    dg = (hc * up * slope).astype(BF16)
    du = (hc * act).astype(BF16)
    return hid, dg, du


def kernel(
    ids, gates, tok_h, cot_h, wg_h, wu_h, wd_h, sg_h, su_h, sd_h,
    o_tok, o_gate, o_rank, o_gg, o_gu, o_gd, o_nrm, o_dn, o_rs, o_sn, o_sdn,
    meta, meta_in, pick, slot_gate, tok, cot, wg, wu, wd, sg, su, sd,
    raw, b0, b1, b2, c0, c1, c2, w0, w1, w2, v0, v1, v2,
    hid_b, dg_b, du_b, rc0, rc1, rc2, rb0, rb1, rb2, s_r0, s_r1, s_r2,
    gpart, gother, g1, g2, g3, stage, nrm, nrm_o, sn, sn_o,
    sh_own, sh_give, sh_got, sh_sum, r0, r1, r2, q0, q1, q2, p1, p2, p3, dnb,
    a_s, a_r, i_s, i_r, d_s, d_r, k_s, k_r, f_s, f_r, x_s, x_r,
    b_s, b_r, y_s, y_r, z_s, z_r, l_s,
    g_s, g_r, t_s, t_r, n_s, n_r, st_s, e_s, e_r, w_s,
):
    out_b, mid, own, oth = (b0, b1, b2), (c0, c1, c2), (w0, w1, w2), (v0, v1, v2)
    rc, rb, s_r = (rc0, rc1, rc2), (rb0, rb1, rb2), (s_r0, s_r1, s_r2)
    me = lax.axis_index("ep")
    h = lax.axis_index("tp")
    mx, my, mz = place(me)
    mate = {"tp": 1 - h}
    width = tok.shape[1] // 2
    half = width // 2

    loads = [
        pltpu.make_async_copy(a, b, w_s.at[i])
        for i, (a, b) in enumerate(
            ((tok_h, tok), (cot_h, cot), (sg_h, sg), (su_h, su), (sd_h, sd), (wg_h, wg), (wu_h, wu), (wd_h, wd))
        )
    ]
    for cp in loads:
        cp.start()
    bar = pltpu.get_barrier_semaphore()

    def axis_peer(axis, d):
        x, y, z = mx, my, mz
        if axis == 0:
            x = lax.rem(x + d, 4)
        elif axis == 1:
            y = lax.rem(y + d, 4)
        else:
            z = lax.rem(z + d, 4)
        return x, y, z, z * 16 + y * 4 + x

    def peer(axis, d):
        return {"ep": axis_peer(axis, d)[3]}

    for axis in range(3):
        for d in range(1, 4):
            pl.semaphore_signal(bar, inc=1, device_id=peer(axis, d), device_id_type=MESH_ID)
    pl.semaphore_signal(bar, inc=1, device_id=mate, device_id_type=MESH_ID)

    def remote(src, dst, s, r, dev):
        return pltpu.make_async_remote_copy(
            src_ref=src, dst_ref=dst, send_sem=s, recv_sem=r, device_id=dev, device_id_type=MESH_ID
        )

    def flat(v):
        return v.reshape(-1, v.shape[-1])

    def blocks(v, *lead):
        return v.reshape(*lead, CAP, v.shape[-1])

    every = slice(None)

    def col(lo, n):
        return pl.ds(pl.multiple_of(h * width + lo, 128), n)

    raw_parts = (
        (0, tok, 0, 768, 0), (1, tok, 768, 256, 0), (1, cot, 0, 256, 256), (2, cot, 256, 768, 0),
    )

    def gather_copies(d):
        cps = []
        for i, (q, src, lo, n, at) in enumerate(raw_parts):
            cps.append((q, remote(
                src.at[:, col(lo, n)], raw.at[pl.ds((d - 1) * 256, 256), pl.ds(R_AT[q] + at, n)],
                a_s.at[d - 1, i], a_r.at[d - 1, i], peer(AXES[q][0], d),
            )))
        return cps

    def meta_copy(q, d):
        return remote(
            meta.at[q, d], meta_in.at[q, d - 1], i_s.at[q, d - 1], i_r.at[q, d - 1], peer(AXES[q][0], d)
        )

    def first_copy(q, d, e):
        return remote(
            out_b[q].at[e - 1, d], mid[q].at[d, e],
            d_s.at[q, d, e - 1], d_r.at[q, d, e - 1], peer(AXES[q][1], e),
        )

    def second_copies(q, c):
        out = []
        for g in (1, 3, 2, 0) if q != 1 else (c,):
            m, o = mid[q], own[q]
            src = (m.at[c, :, g], m.at[:, :, c], m.at[:, c, g])[q]
            dst = (o.at[c, :, g], o.at[c], o.at[c, g])[q]
            if g == 0:
                out.append((g, pltpu.make_async_copy(src, dst, k_s.at[q, c, 0])))
            else:
                out.append((g, remote(src, dst, k_s.at[q, c, g], k_r.at[q, c, g], peer(AXES[q][2], g))))
        return out

    def forward(q, c):
        return remote(own[q].at[c], oth[q].at[c], f_s.at[q, c], f_r.at[q, c], mate)

    firsts = set()

    def second(q, c):
        for d in (c,) if q == 0 else range(4):
            for e in (c,) if q == 2 else range(4):
                if e > 0 and (q, d, e) not in firsts:
                    firsts.add((q, d, e))
                    first_copy(q, d, e).wait_recv()
        for _, cp in second_copies(q, c):
            cp.start()

    n_tok = tok.shape[0]
    earlier = lax.broadcasted_iota(jnp.int32, (n_tok, n_tok), 0)
    later = lax.broadcasted_iota(jnp.int32, (n_tok, n_tok), 1)
    before = jnp.where(later > earlier, 1.0, 0.0).astype(BF16)
    for q in range(3):
        order = named_in_order(me, q, n_tok)
        named = jnp.zeros((NEP, n_tok), F32)
        gate_t = jnp.zeros((NEP, n_tok), F32)
        for j in range(4):
            hit = ids[j:j + 1] == order
            named = jnp.where(hit, 1.0, named)
            gate_t = jnp.where(hit, gates[j:j + 1], gate_t)
        rank_t = jnp.where(named > 0.0, nn(named.astype(BF16), before), -1.0)
        if q == 0:
            o_rank[...] = rank_t
        for d in range(4):
            meta[q, d, 0] = rank_t[d * 16:(d + 1) * 16]
            meta[q, d, 1] = gate_t[d * 16:(d + 1) * 16]

    for cp in loads[:2]:
        cp.wait()
    pl.semaphore_wait(bar, 10)
    sends = []
    for d in (1, 3, 2):
        for q in range(3):
            sends.append(meta_copy(q, d))
        sends.extend(cp for _, cp in gather_copies(d))
    n_near = 2 * len(sends) // 3
    for cp in sends[:n_near]:
        cp.start()

    slot_no = lax.broadcasted_iota(jnp.int32, (CAP, n_tok), 0).astype(F32)

    def place_rows(q, d, with_gate):
        ref = meta.at[q, 0] if d == 0 else meta_in.at[q, d - 1]
        for k in range(16):
            filled = ref[0, k:k + 1] == slot_no
            pick[k * CAP:(k + 1) * CAP] = jnp.where(filled, 1.0, 0.0).astype(BF16)
            if with_gate:
                slot_gate[k * CAP:(k + 1) * CAP] = jnp.sum(
                    jnp.where(filled, ref[1, k:k + 1], 0.0), axis=1, keepdims=True
                )

    def put(q, d, cols, v):
        v = blocks(v, 4, 4).astype(BF16)
        mid[q][d, 0, :, :, cols] = v[0]
        for e in range(1, 4):
            out_b[q][e - 1, d, :, :, cols] = v[e]

    for cp in loads[2:]:
        cp.wait()
    gp = nn(tok[...], sg[...])
    up = nn(tok[...], su[...])
    hc = nt(cot[...], sd[...])
    s_hid, s_dg, s_du = nonlinear(gp, up, hc)
    tile = 512
    tiles = tok.shape[1] // tile
    for i in range(tiles):
        cs = slice(i * tile, (i + 1) * tile)
        t_t = tok[:, cs]
        r0[i] = tn(t_t, s_dg).astype(BF16)
        r1[i] = tn(t_t, s_du).astype(BF16)
        r2[4 * i:4 * i + 4] = tn(cot[:, cs], s_hid).astype(BF16).reshape(4, 128, 256)

    def rs_copies(phase):
        out = []
        for d in (1, 3, 2):
            for a in range(3):
                axis = AXES[a][phase]
                x, y, z, dev = axis_peer(axis, d)
                if phase == 0:
                    src = (r0.at[z], r1.at[:, pl.ds(pl.multiple_of(y * 128, 128), 128)],
                           r2.at[:, pl.ds(pl.multiple_of(x * 32, 32), 32)])[a]
                    dst = (q0, q1, q2)[a].at[d - 1]
                elif phase == 1:
                    src = (p1.at[0, pl.ds(pl.multiple_of(y * 4, 4), 4)], p1.at[1, pl.ds(pl.multiple_of(x * 4, 4), 4)],
                           p1.at[2, pl.ds(pl.multiple_of(z * 4, 4), 4)])[a]
                    dst = p2.at[a, d]
                else:
                    src = p2.at[a, 0, (x, z, y)[a]]
                    dst = p3.at[a, d - 1]
                i = (phase * 3 + d - 1) * 3 + a
                out.append(remote(src, dst, t_s.at[i], t_r.at[i], {"ep": dev}))
        return out

    def produce(d):
        for q in range(3):
            if d > 0:
                meta_copy(q, d).wait_recv()
                for qq, cp in gather_copies(d):
                    if qq == q:
                        cp.wait_recv()
            place_rows(q, d, q > 0)
            for qq, src, lo, n, at in raw_parts:
                if qq != q:
                    continue
                for j in range(0, n, 256):
                    if d == 0:
                        x = src[:, col(lo + j, 256)]
                    else:
                        x = raw[(d - 1) * 256:d * 256, R_AT[q] + at + j:R_AT[q] + at + j + 256]
                    v = nn(pick[...], x)
                    if src is cot:
                        v = slot_gate[...] * v
                    put(q, d, slice(at + j, at + j + 256), v)
            for e in range(1, 4):
                first_copy(q, d, e).start()

    produce(0)
    for cp in sends[n_near:]:
        cp.start()
    for i in range(2):
        cols = pl.ds(pl.multiple_of(h * width + i * half, 128), half)
        r = pl.ds(pl.multiple_of(h * width + i * half, 128), half)
        sh_own[:, i * half:(i + 1) * half] = (
            nt(s_dg, sg[r]) + nt(s_du, su[r])
        ).astype(BF16)
        r = pl.ds(pl.multiple_of((1 - h) * width + i * half, 128), half)
        sh_give[:, i * half:(i + 1) * half] = (
            nt(s_dg, sg[r]) + nt(s_du, su[r])
        ).astype(BF16)
    sh_cp = remote(sh_give, sh_got, e_s.at[0], e_r.at[0], mate)
    sh_cp.start()

    produce(1)
    produce(3)
    produce(2)
    rs0 = rs_copies(0)
    second(2, 0)
    second(0, 0)

    for q, c in ((1, 0), (0, 1), (1, 1), (1, 3), (2, 1), (1, 2), (0, 3), (2, 3)):
        second(q, c)

    def arrive(c):
        for q in range(3):
            for g, cp in second_copies(q, c):
                if g > 0:
                    cp.wait_recv()
                else:
                    cp.wait()
            forward(q, c).start()

    def cross(c):
        out = []
        for i in range(4):
            buf, at = give_at(c, i)
            dst = raw.at[pl.ds((c // 2) * CR, CR), pl.ds((c % 2) * width + i * 256, 256)]
            out.append(remote(buf.at[pl.ds(at, CR)], dst, x_s.at[c, i], x_r.at[c, i], mate))
        return out

    def give_at(c, i):
        n = ORDER.index(c) % 2 * 4 + i
        return (sg, su)[n // 5], n % 5 * CR

    def back_at(q, c):
        if q == 0:
            return out_b[0], c % 3, 384 * (c // 3)
        if c == 3:
            return out_b[2], q - 1 if q == 1 else 1, 256
        return out_b[q], c, 0

    def rows_of(base, lo, n):
        return pl.ds(pl.multiple_of(base * width + lo, 128), n)

    def compute(c):
        rows = pl.ds(c * CR, CR)
        for q in range(3):
            forward(q, c).wait_recv()
        gp = up = hc = None
        for base, buf in ((h, own), (1 - h, oth)):
            for lo, n, x in ((0, 768, flat(buf[0][c])), (768, 256, flat(buf[1][c, :, :, :, :256]))):
                r = rows_of(base, lo, n)
                g, u = nn(x, wg[r]), nn(x, wu[r])
                gp, up = (g, u) if gp is None else (gp + g, up + u)
            for lo, n, x in ((0, 256, flat(buf[1][c, :, :, :, 256:])), (256, 768, flat(buf[2][c]))):
                t = nt(x, wd[:, rows_of(base, lo, n)])
                hc = t if hc is None else hc + t
        hid, dg, du = nonlinear(gp, up, hc)
        hid_b[rows] = hid
        dg_b[rows] = dg
        du_b[rows] = du
        gsum = jnp.sum(hid.astype(F32) * hc, axis=1, keepdims=True).reshape(BLK, CAP, 1)
        lane = lax.broadcasted_iota(jnp.int32, (BLK, CAP, 128), 2)
        rank = lax.broadcasted_iota(jnp.int32, (BLK, CAP, 128), 1)
        packed = jnp.sum(jnp.where(lane == rank, gsum, 0.0), axis=1)
        for i in range(BLK):
            gpart[c, i // 4, i % 4] = packed[i:i + 1]
        if ORDER.index(c) >= 2:
            for cp in cross(ORDER[ORDER.index(c) - 2]):
                cp.wait_send()
        for i, cp in enumerate(cross(c)):
            buf, at = give_at(c, i)
            r = pl.ds(pl.multiple_of((1 - h) * width + i * 256, 256), 256)
            buf[at:at + CR] = (nt(dg, wg[r]) + nt(du, wu[r])).astype(BF16)
            cp.start()
        for q in range(3):
            r = rows_of(h, B_AT[q], BACK[q])
            buf, b, lo = back_at(q, c)
            buf[b, :, :, :, lo:lo + BACK[q]] = blocks(nt(dg, wg[r]) + nt(du, wu[r]), 4, 4).astype(BF16)

    def back_copies(q, c):
        out = []
        buf, b, lo = back_at(q, c)
        src = buf.at[b, :, :, :, pl.ds(lo, BACK[q])]
        for g in (1, 3, 2, 0) if q != 1 else (c,):
            s_g = (src.at[:, g], src, src.at[g])[q]
            v = rc[q]
            dst = (v.at[c, :, g], v.at[:, :, c], v.at[:, c, g])[q]
            if g == 0:
                out.append((g, pltpu.make_async_copy(s_g, dst, l_s.at[q, c])))
            else:
                to = peer(AXES[q][2], 4 - g)
                out.append((g, remote(s_g, dst, b_s.at[q, c, g], b_r.at[q, c, g], to)))
        return out

    def finish(c):
        for cp in cross(c):
            cp.wait_recv()
        for q in range(3):
            n = BACK[q]
            buf, b, lo = back_at(q, c)
            at = c % 2 * width + B_AT[q]
            buf[b, :, :, :, lo:lo + n] = (
                buf[b, :, :, :, lo:lo + n].astype(F32)
                + blocks(raw[(c // 2) * CR:(c // 2 + 1) * CR, at:at + n].astype(F32), 4, 4)
            ).astype(BF16)
        for q in range(3):
            for _, cp in back_copies(q, c):
                cp.start()

    def back2_copies(q, c):
        out = []
        v, w = rc[q], rb[q]
        for e in (1, 3, 2, 0) if q != 2 else (c,):
            at = ((c, e), (every, e, c), (every, e))[q]
            if e == 0:
                out.append((e, pltpu.make_async_copy(v.at[at], w.at[at], l_s.at[q, 4 + c])))
            else:
                to = peer(AXES[q][1], 4 - e)
                out.append((e, remote(v.at[at], w.at[at], y_s.at[q, c, e], y_r.at[q, c, e], to)))
        return out

    def legs(c):
        for q in (1, 2, 0):
            for g, cp in back_copies(q, c):
                if g > 0:
                    cp.wait_recv()
                else:
                    cp.wait()
            for _, cp in back2_copies(q, c):
                cp.start()

    for q in range(3):
        for d in range(4):
            for e in range(1, 4):
                first_copy(q, d, e).wait_send()
    for n, c in enumerate(ORDER):
        arrive(c)
        for q, cc in ((), ((0, 2), (2, 2)), (), ())[n]:
            second(q, cc)
        for a in ((), (0,), (1, 2), ())[n]:
            for cp in rs0[a::3]:
                cp.start()
        if n >= 1:
            finish(ORDER[n - 1])
        compute(c)
        if n == 2:
            legs(0)
    g_cp = remote(gpart, gother, e_s.at[1], e_r.at[1], mate)
    g_cp.start()
    finish(ORDER[-1])
    legs(1)

    def leg2_done(q, c):
        for e, cp in back2_copies(q, c):
            if e > 0:
                cp.wait_recv()
            else:
                cp.wait()

    def back3_copy(q, d):
        return remote(
            raw.at[pl.ds((d - 1) * 256, 256), pl.ds(R_AT[q], BACK[q])], s_r[q].at[d - 1],
            z_s.at[q, d], z_r.at[q, d], peer(AXES[q][0], 4 - d),
        )

    def leg3(q, d):
        place_rows(q, d, False)
        v = tn(pick[...], flat(rb[q][d]))
        if d > 0:
            raw[(d - 1) * 256:d * 256, R_AT[q]:R_AT[q] + BACK[q]] = v.astype(BF16)
            back3_copy(q, d).start()
        else:
            sh_sum[:, B_AT[q]:B_AT[q] + BACK[q]] = v

    def near_rows():
        for d in (0, 1, 3):
            leg2_done(0, d)
            leg3(0, d)

    def far_rows():
        for q in (1, 2):
            for c in ORDER:
                leg2_done(q, c)
            for d in (1, 3, 2, 0):
                leg3(q, d)
        leg2_done(0, 2)
        leg3(0, 2)

    def f(v):
        return v.astype(F32)

    def scatter2():
        for cp in rs0:
            cp.wait()
        s0 = f(r0[mz]) + f(q0[0]) + f(q0[1]) + f(q0[2])
        p1[0] = s0.reshape(16, 32, 256).astype(BF16)
        s1 = (f(r1[:, pl.ds(pl.multiple_of(my * 128, 128), 128)]) + f(q1[0]) + f(q1[1]) + f(q1[2])).reshape(4, 4, 32, 256)
        for i in range(4):
            for j in range(4):
                p1[1, 4 * j + i] = s1[i, j].astype(BF16)
        s2 = f(r2[:, pl.ds(pl.multiple_of(mx * 32, 32), 32)]) + f(q2[0]) + f(q2[1]) + f(q2[2])
        p1[2] = s2.astype(BF16)
        for cp in rs_copies(1):
            cp.start()

    def scatter3():
        for cp in rs_copies(1):
            cp.wait()
        for a in range(3):
            own_i = (my, mx, mz)[a]
            p2[a, 0] = (
                f(p1[a, pl.ds(pl.multiple_of(own_i * 4, 4), 4)]) + f(p2[a, 1]) + f(p2[a, 2]) + f(p2[a, 3])
            ).astype(BF16)
        for cp in rs_copies(2):
            cp.start()

    gates_on = (gother, g1, g2, g3)

    def gate_copies(leg):
        out = []
        for g in range(1, 4):
            at = ((every, every, g), (every, g), (g,))[leg]
            src, dst = gates_on[leg].at[at], gates_on[leg + 1].at[at]
            out.append(remote(src, dst, g_s.at[leg, g], g_r.at[leg, g], peer(leg, 4 - g)))
        return out

    def gate_leg(leg):
        if leg == 0:
            g_cp.wait()
            gother[...] = gpart[...] + gother[...]
        else:
            for cp in gate_copies(leg - 1):
                cp.wait()
        at = ((every, every, 0), (every, 0), (0,))[leg]
        gates_on[leg + 1][at] = gates_on[leg][at]
        for cp in gate_copies(leg):
            cp.start()

    sn_cp = remote(sn, sn_o, e_s.at[3], e_r.at[3], mate)

    def spread(leg):
        return [
            remote(dnb.at[leg, 0], dnb.at[leg, g], n_s.at[leg, g], n_r.at[leg, g], peer(leg, g))
            for g in range(1, 4)
        ]

    def spread_leg(leg):
        if leg > 0:
            for cp in spread(leg - 1):
                cp.wait()
            dnb[leg, 0] = dnb[leg - 1, 0] + dnb[leg - 1, 1] + dnb[leg - 1, 2] + dnb[leg - 1, 3]
        if leg < 3:
            for cp in spread(leg):
                cp.start()

    def scatter_end():
        for cp in rs_copies(2):
            cp.wait()
        for a in range(3):
            own_i = (mx, mz, my)[a]
            v = f(p2[a, 0, own_i]) + f(p3[a, 0]) + f(p3[a, 1]) + f(p3[a, 2])
            o_rs[a] = v
            if a < 2:
                sn[a] = jnp.broadcast_to(jnp.sum(v * v, axis=1, keepdims=True), (32, 128))
            else:
                dnb[0, 0] = jnp.sum(v * v, axis=0, keepdims=True)
        sn_cp.start()
        spread_leg(0)

    ones = jnp.ones((8, 256), F32)

    def row_norm(g):
        return lax.dot_general(
            ones, g * g, (((1,), (1,)), ((), ())), preferred_element_type=F32, precision=lax.Precision.HIGHEST
        )

    n_t = width // 256

    def stage_copies(step, slot, f0):
        fr = pl.ds(f0, 256)
        return (
            pltpu.make_async_copy(stage.at[slot, 0], o_gg.at[fr], st_s.at[slot, 0]),
            pltpu.make_async_copy(stage.at[slot, 1], o_gu.at[fr], st_s.at[slot, 1]),
            pltpu.make_async_copy(stage.at[slot, 2], o_gd.at[:, fr], st_s.at[slot, 2]),
        )

    hid_all = hid_b[...]
    dn = jnp.zeros((8, 256), F32)
    pending = [None, None]
    AFTER = {
        0: (functools.partial(legs, 3), functools.partial(gate_leg, 0)),
        1: (functools.partial(legs, 2), scatter2),
        2: (near_rows, functools.partial(gate_leg, 1)),
        3: (far_rows, scatter3),
        4: (functools.partial(gate_leg, 2),),
        5: (scatter_end,),
        6: (functools.partial(spread_leg, 1),),
        7: (functools.partial(spread_leg, 2),),
    }
    for step in range(2 * n_t):
        slot = step % 2
        buf = own if step < n_t else oth
        i = step % n_t
        base = h if step < n_t else 1 - h
        f0 = pl.multiple_of(base * width + i * 256, 256)
        if pending[slot] is not None:
            for cp in pending[slot]:
                cp.wait()
        lhs = flat(buf[0][..., i * 256:(i + 1) * 256] if i < 3 else buf[1][..., :256])
        rhs = flat(buf[1][..., 256:] if i == 0 else buf[2][..., (i - 1) * 256:i * 256])
        grad1 = tn(lhs, dg_b[...])
        stage[slot, 0] = grad1
        nrm[0:8, pl.ds(f0, 256)] = row_norm(grad1)
        grad2 = tn(lhs, du_b[...])
        stage[slot, 1] = grad2
        nrm[8:16, pl.ds(f0, 256)] = row_norm(grad2)
        grad3 = tn(hid_all, rhs)
        stage[slot, 2] = grad3
        dn = dn + row_norm(grad3)
        pending[slot] = stage_copies(step, slot, f0)
        for cp in pending[slot]:
            cp.start()
        for fn in AFTER.get(step, ()):
            fn()
    o_dn[...] = dn
    nrm_cp = remote(nrm, nrm_o, e_s.at[2], e_r.at[2], mate)
    nrm_cp.start()

    nrm_cp.wait()
    o_nrm[...] = nrm[...] + nrm_o[...]
    sn_cp.wait()
    o_sn[...] = sn[...] + sn_o[...]
    sh_cp.wait()
    for cp in gate_copies(2):
        cp.wait()
    for k in range(NEP):
        o_gate[k:k + 1] = g3[k // 16, k // 4 % 4, k % 4]
    for q in range(3):
        cs = slice(B_AT[q], B_AT[q] + BACK[q])
        v = sh_sum[:, cs] + (f(sh_own[:, cs]) + f(sh_got[:, cs]))
        for d in range(1, 4):
            back3_copy(q, d).wait()
            v = v + f(s_r[q][d - 1])
        o_tok[:, cs] = v.astype(BF16)

    spread_leg(3)
    o_sdn[...] = dnb[3, 0]
    for cp in sends:
        cp.wait_send()
    for q in range(3):
        for c in range(CHUNKS):
            forward(q, c).wait_send()
            for g, cp in second_copies(q, c) + back_copies(q, c):
                if g > 0:
                    cp.wait_send()
            for e, cp in back2_copies(q, c):
                if e > 0:
                    cp.wait_send()
    for c in ORDER[2:]:
        for cp in cross(c):
            cp.wait_send()
    for cps in pending:
        for cp in cps:
            cp.wait()


def tail(
    ids, gates, rank, gate_sum, tok_in, nrm, dn, rs, sn, sdn, gg, gu, gd,
    o_tok, o_gate, o_gg, o_gu, o_gd, o_sg, o_su, o_sd, o_gn, o_un, o_dn, o_sgn, o_sun, o_sdn,
    bg, bu, bd, i_s, o_s,
):
    rows = bd.shape[0]
    parts = []
    for a, (src, buf, dst) in enumerate(((gg, bg, o_gg), (gu, bu, o_gu))):
        for i in range(2):
            r = pl.ds(i * 1024, 1024)
            parts.append((src.at[r], buf.at[r], dst.at[0, r]))
    for i in range(2):
        r = pl.ds(i * 128, 128)
        parts.append((gd.at[r], bd.at[r], o_gd.at[0, r]))
    ins = [pltpu.make_async_copy(a, b, i_s.at[i]) for i, (a, b, _) in enumerate(parts)]
    outs = [pltpu.make_async_copy(b, c, o_s.at[i]) for i, (_, b, c) in enumerate(parts)]
    for cp in ins:
        cp.start()
    o_tok[...] = tok_in[...]
    order = named_in_order(lax.axis_index("ep"), 0, rank.shape[1])
    value = jnp.zeros(rank.shape, F32)
    for r in range(CAP):
        value = jnp.where(rank[...] == float(r), gate_sum[:, r:r + 1], value)
    for j in range(4):
        hit = ids[j:j + 1] == order
        total = jnp.sum(jnp.where(hit, value, 0.0), axis=0, keepdims=True)
        o_gate[j:j + 1] = total / gates[j:j + 1]
    o_sg[...] = rs[0]
    o_su[...] = rs[1]
    o_sd[...] = rs[2]
    o_gn[...] = nrm[0:1]
    o_un[...] = nrm[8:9]
    o_dn[...] = dn[0:1]
    o_sgn[...] = sn[0].T[0:1]
    o_sun[...] = sn[1].T[0:1]
    o_sdn[...] = sdn[...]
    for a, b in zip(ins, outs):
        a.wait()
        b.start()
    for b in outs:
        b.wait()


def local(tokens, expert_ids, gates, cotangent, w_gate, w_up, w_down, sh_gate, sh_up, sh_down):
    rows, width = tokens.shape
    ids_t, gates_t = expert_ids.T, gates.T

    vm = pl.BlockSpec(memory_space=pltpu.VMEM)
    hbm = pl.BlockSpec(memory_space=pl.ANY)
    half = width // 2
    dma = pltpu.SemaphoreType.DMA
    out = pl.pallas_call(
        kernel,
        out_shape=(
            jax.ShapeDtypeStruct((rows, half), BF16),
            jax.ShapeDtypeStruct((NEP, 128), F32),
            jax.ShapeDtypeStruct((NEP, rows), F32),
            jax.ShapeDtypeStruct((width, 256), F32),
            jax.ShapeDtypeStruct((width, 256), F32),
            jax.ShapeDtypeStruct((256, width), F32),
            jax.ShapeDtypeStruct((16, width), F32),
            jax.ShapeDtypeStruct((8, 256), F32),
            jax.ShapeDtypeStruct((3, 32, 256), F32),
            jax.ShapeDtypeStruct((2, 32, 128), F32),
            jax.ShapeDtypeStruct((1, 256), F32),
        ),
        in_specs=[vm] * 2 + [hbm] * 8,
        out_specs=(vm, vm, vm, hbm, hbm, hbm, vm, vm, vm, vm, vm),
        scratch_shapes=[
            pltpu.VMEM((3, 4, 2, 16, rows), F32),
            pltpu.VMEM((3, 3, 2, 16, rows), F32),
            pltpu.VMEM((CR, rows), BF16),
            pltpu.VMEM((CR, 1), F32),
            pltpu.VMEM((rows, width), BF16),
            pltpu.VMEM((rows, width), BF16),
            pltpu.VMEM((width, 256), BF16),
            pltpu.VMEM((width, 256), BF16),
            pltpu.VMEM((256, width), BF16),
            pltpu.VMEM((width, 256), BF16),
            pltpu.VMEM((width, 256), BF16),
            pltpu.VMEM((256, width), BF16),
            pltpu.VMEM((3 * rows, width), BF16),
            *[pltpu.VMEM((3, 4, 4, CAP, n), BF16) for n in WIDE],
            *[pltpu.VMEM((4, 4, 4, CAP, n), BF16) for n in WIDE],
            *[pltpu.VMEM((4, 4, 4, CAP, n), BF16) for n in WIDE],
            *[pltpu.VMEM((4, 4, 4, CAP, n), BF16) for n in WIDE],
            pltpu.VMEM((ROWS, 256), BF16),
            pltpu.VMEM((ROWS, 256), BF16),
            pltpu.VMEM((ROWS, 256), BF16),
            *[pltpu.VMEM((4, 4, 4, CAP, n), BF16) for n in BACK],
            *[pltpu.VMEM((4, 4, 4, CAP, n), BF16) for n in BACK],
            *[pltpu.VMEM((3, rows, n), BF16) for n in BACK],
            *[pltpu.VMEM((4, 4, 4, 1, 128), F32)] * 5,
            pltpu.VMEM((2, 3, 256, 256), F32),
            pltpu.VMEM((16, width), F32),
            pltpu.VMEM((16, width), F32),
            pltpu.VMEM((2, 32, 128), F32),
            pltpu.VMEM((2, 32, 128), F32),
            pltpu.VMEM((rows, half), BF16),
            pltpu.VMEM((rows, half), BF16),
            pltpu.VMEM((rows, half), BF16),
            pltpu.VMEM((rows, half), F32),
            pltpu.VMEM((4, 512, 256), BF16),
            pltpu.VMEM((4, 512, 256), BF16),
            pltpu.VMEM((16, 128, 256), BF16),
            pltpu.VMEM((3, 512, 256), BF16),
            pltpu.VMEM((3, 4, 128, 256), BF16),
            pltpu.VMEM((3, 16, 32, 256), BF16),
            pltpu.VMEM((3, 16, 32, 256), BF16),
            pltpu.VMEM((3, 4, 4, 32, 256), BF16),
            pltpu.VMEM((3, 3, 32, 256), BF16),
            pltpu.VMEM((4, 4, 1, 256), F32),
            dma((3, 4)), dma((3, 4)),
            dma((3, 3)), dma((3, 3)),
            dma((3, 4, 3)), dma((3, 4, 3)),
            dma((3, 4, 4)), dma((3, 4, 4)),
            dma((3, 4)), dma((3, 4)),
            dma((CHUNKS, 4)), dma((CHUNKS, 4)),
            dma((3, CHUNKS, 4)), dma((3, CHUNKS, 4)),
            dma((3, CHUNKS, 4)), dma((3, CHUNKS, 4)),
            dma((3, 4)), dma((3, 4)),
            dma((3, 8)),
            dma((3, 4)), dma((3, 4)),
            dma((27,)), dma((27,)),
            dma((3, 4)), dma((3, 4)),
            dma((2, 3)),
            dma((4,)), dma((4,)),
            dma((8,)),
        ],
        compiler_params=pltpu.CompilerParams(
            collective_id=0, has_side_effects=True, vmem_limit_bytes=67043328
        ),
    )(ids_t, gates_t, tokens, cotangent, w_gate[0], w_up[0], w_down[0], sh_gate, sh_up, sh_down)
    tok_grad, gate_sum, rank, gg, gu, gd, nrm, dn, rs, sn, sdn = out
    res = pl.pallas_call(
        tail,
        out_shape=(
            jax.ShapeDtypeStruct((rows, half), BF16),
            jax.ShapeDtypeStruct((4, rows), F32),
            jax.ShapeDtypeStruct((1, width, 256), F32),
            jax.ShapeDtypeStruct((1, width, 256), F32),
            jax.ShapeDtypeStruct((1, 256, width), F32),
            jax.ShapeDtypeStruct((32, 256), F32),
            jax.ShapeDtypeStruct((32, 256), F32),
            jax.ShapeDtypeStruct((32, 256), F32),
            jax.ShapeDtypeStruct((1, width), F32),
            jax.ShapeDtypeStruct((1, width), F32),
            jax.ShapeDtypeStruct((1, 256), F32),
            jax.ShapeDtypeStruct((1, 32), F32),
            jax.ShapeDtypeStruct((1, 32), F32),
            jax.ShapeDtypeStruct((1, 256), F32),
        ),
        in_specs=[vm] * 10 + [hbm] * 3,
        out_specs=(vm, vm, hbm, hbm, hbm) + (vm,) * 9,
        scratch_shapes=[
            pltpu.VMEM((width, 256), F32),
            pltpu.VMEM((width, 256), F32),
            pltpu.VMEM((256, width), F32),
            dma((6,)), dma((6,)),
        ],
    )(ids_t, gates_t, rank, gate_sum, tok_grad, nrm, dn, rs, sn, sdn, gg, gu, gd)
    return (res[0], res[1].T) + res[2:7] + (res[7].T,) + res[8:11] + (res[11][0], res[12][0], res[13][0])


def solution(mesh):
    placed = (
        P("ep", None),
        P("ep", None),
        P("ep", None),
        P("ep", None),
        P("ep", None, "tp"),
        P("ep", None, "tp"),
        P("ep", "tp", None),
        P(None, "tp"),
        P(None, "tp"),
        P("tp", None),
    )
    return jax.shard_map(
        local,
        mesh=mesh,
        in_specs=placed,
        out_specs=(
            P("ep", "tp"),
            P("ep", None),
            P("ep", None, "tp"),
            P("ep", None, "tp"),
            P("ep", "tp", None),
            P("ep", "tp"),
            P("ep", "tp"),
            P("tp", "ep"),
            P("ep", None),
            P("ep", None),
            P("ep", "tp"),
            P("ep"),
            P("ep"),
            P("tp"),
        ),
        check_vma=False,
    )
```
